512 devices in a mesh: rep: 2 (over z_hi), fs: 32 (over z_lo, y), tp: 8 (over x, core).
Axes of the slice: x: 4, y: 4, z: 16 (z_hi: 2, z_lo: 8; z = z_hi * 8 + z_lo), core: 2. Of those that a mesh axis runs over, the one named last changes fastest.
Arguments:
- tokens: bfloat16 [16384, 2048], P(('rep', 'fs')), may hold values from -6 to 6
- first_gain: float32 [2048], replicated, may hold values from 0.1 to 1.9
- value_weight: float32 [2048, 1024], P('fs', 'tp'), may hold values from -0.125 to 0.125
- gate_weight: float32 [2048, 1024], P('fs', 'tp'), may hold values from -0.125 to 0.125
- value_scale: float32 [1024], P('tp'), may hold values from 0.5 to 2
- gate_scale: float32 [1024], P('tp'), may hold values from 0.5 to 2
- conv_taps: float32 [31, 1024], P(None, 'tp'), may hold values from -7 to 7
- chan_gain: float32 [1024], P('tp'), may hold values from 0.1 to 1.9
- mixout_weight: float32 [1024, 2048], P('tp', 'fs'), may hold values from -0.1875 to 0.1875
- mixout_scale: float32 [2048], P('fs'), may hold values from 0.5 to 2
- second_gain: float32 [2048], replicated, may hold values from 0.1 to 1.9
- up_weight: float32 [2048, 8192], P('fs', 'tp'), may hold values from -0.125 to 0.125
- up_scale: float32 [8192], P('tp'), may hold values from 0.5 to 2
- down_weight: float32 [8192, 2048], P('tp', 'fs'), may hold values from -0.0625 to 0.0625
- down_scale: float32 [2048], P('fs'), may hold values from 0.5 to 2
Outputs:
- layer_out: bfloat16 [16384, 2048], P(('rep', 'fs'))
The draws below stay inside these ranges and needn't reach their ends.
All inputs are finite; a program needn't handle non-finite values.
Results may differ from the reference program's by a relative error of at most 0.025.
Values may be sent and summed in bfloat16 or wider, within the bound.
No kernel may reach another device: no remote copies, remote signals or barrier semaphores. Data moves between devices by JAX's collectives and lax.ppermute only.
A program may use at most 128 MiB of HBM per device.

```python
import math
import jax
import jax.numpy as jnp
from jax import lax

D = 2048
CHANNELS = 1024
FF = 8192
CONV_K = 31
SEQ_LEN = 128
TOKENS = 16384
N_TP = 8


def draw_conv_taps(key, part):
    first, second = jax.random.split(jax.random.fold_in(key, 11))
    channel = jnp.arange(CHANNELS).astype(jnp.float32)
    rise = jnp.exp(jnp.log(6.0) * channel / max(CHANNELS - 1, 1))
    base = jnp.clip(jax.random.normal(first, (CONV_K, CHANNELS), jnp.float32), -4.0, 4.0)
    rough = jax.random.uniform(second, (CHANNELS,), jnp.float32, 0.5, 1.5)
    return (base * CONV_K ** (-0.5) * rise * rough).astype(jnp.float32)


def levels(key, dims, cuts, low, high):
    def one(dim, blocks):
        heights = jax.random.uniform(jax.random.fold_in(jax.random.fold_in(key, 6), dim), (blocks,), jnp.float32, low / len(cuts), high / len(cuts))
        return jnp.repeat(jnp.exp(heights), dims[dim] // blocks).reshape((-1,) + (1,) * (len(dims) - dim - 1))

    level = one(*cuts[0])
    for cut in cuts[1:]:
        level = level * one(*cut)
    return level


def scatter_about(own_key, extent, scale, reach, cuts=(), kind=jnp.bfloat16):
    factor_of = levels(own_key, extent, cuts, -0.22, 0.18) if cuts else 1.0
    values = jax.random.normal(own_key, extent, jnp.float32) * scale * factor_of
    return jnp.minimum(jnp.maximum(values, -reach), reach).astype(kind)


def setup_inputs(seed: int = 0) -> dict:
    keys = jax.random.split(jax.random.key(seed), 16)
    tokens = scatter_about(keys[0], (TOKENS, D), 1.0, 6.0, ((0, 64),))
    first_gain = jnp.clip(1.0 + 0.18 * jax.random.normal(keys[1], (D,), jnp.float32), 0.1, 1.9)
    value_weight = scatter_about(keys[2], (D, CHANNELS), D ** -0.5, 0.125, ((0, 32), (1, 8)), jnp.float32)
    gate_weight = scatter_about(keys[3], (D, CHANNELS), D ** -0.5, 0.125, ((0, 32), (1, 8)), jnp.float32)
    value_scale = jnp.clip(jnp.exp(math.log(2.0) - 1.3862944 * jax.random.uniform(keys[4], (CHANNELS,), jnp.float32) ** levels(keys[4], (CHANNELS,), ((0, 8),), -0.2, 0.2)), 0.5, 2.0)
    gate_scale = jnp.clip(jnp.exp(math.log(2.0) - 1.3862944 * jax.random.uniform(keys[5], (CHANNELS,), jnp.float32) ** levels(keys[5], (CHANNELS,), ((0, 8),), -0.2, 0.2)), 0.5, 2.0)
    conv_taps = draw_conv_taps(jax.random.fold_in(keys[15], 71), 0)
    chan_gain = jnp.clip(1.0 + 0.18 * jax.random.normal(keys[7], (CHANNELS,), jnp.float32), 0.1, 1.9)
    mixout_weight = scatter_about(keys[8], (CHANNELS, D), CHANNELS ** -0.5, 0.1875, ((0, 8), (1, 32)), jnp.float32)
    mixout_scale = jnp.clip(jnp.exp(math.log(2.0) - 1.3862944 * jax.random.uniform(keys[9], (D,), jnp.float32) ** levels(keys[9], (D,), ((0, 32),), -0.2, 0.2)), 0.5, 2.0)
    second_gain = jnp.clip(1.0 + 0.18 * jax.random.normal(keys[10], (D,), jnp.float32), 0.1, 1.9)
    up_weight = scatter_about(keys[11], (D, FF), D ** -0.5, 0.125, ((0, 32), (1, 8)), jnp.float32)
    up_scale = jnp.clip(jnp.exp(math.log(2.0) - 1.3862944 * jax.random.uniform(keys[12], (FF,), jnp.float32) ** levels(keys[12], (FF,), ((0, 8),), -0.2, 0.2)), 0.5, 2.0)
    down_weight = scatter_about(keys[13], (FF, D), FF ** -0.5, 0.0625, ((0, 8), (1, 32)), jnp.float32)
    down_scale = jnp.clip(jnp.exp(math.log(2.0) - 1.3862944 * jax.random.uniform(keys[14], (D,), jnp.float32) ** levels(keys[14], (D,), ((0, 32),), -0.2, 0.2)), 0.5, 2.0)
    return {"tokens": tokens, "first_gain": first_gain, "value_weight": value_weight, "gate_weight": gate_weight, "value_scale": value_scale, "gate_scale": gate_scale, "conv_taps": conv_taps, "chan_gain": chan_gain, "mixout_weight": mixout_weight, "mixout_scale": mixout_scale, "second_gain": second_gain, "up_weight": up_weight, "up_scale": up_scale, "down_weight": down_weight, "down_scale": down_scale}


def rms_rows(rows, gain):
    values = rows.astype(jnp.float32)
    scaled = values * lax.rsqrt(lax.optimization_barrier(jnp.mean(values * values, axis=-1, keepdims=True)) + 1e-05)
    return (scaled * gain).astype(jnp.bfloat16)

def rounded(scale):
    return lax.optimization_barrier(scale.astype(jnp.bfloat16)).astype(jnp.float32)

def causal_conv(signal, taps):
    width = signal.shape[1]
    seqs = signal.reshape(-1, SEQ_LEN, width)
    result = lax.conv_general_dilated(seqs, taps[:, None, :], (1,), [(taps.shape[0] - 1, 0)], dimension_numbers=('NWC', 'WIO', 'NWC'), feature_group_count=width, precision=lax.Precision.HIGHEST)
    return result.reshape(signal.shape)

def block_sum(left, right, scale):
    inner = left.shape[1] // N_TP
    total = jnp.zeros((left.shape[0], right.shape[1]), jnp.float32)
    for block in range(N_TP):
        term = jnp.dot(left[:, block * inner:(block + 1) * inner], right[block * inner:(block + 1) * inner], preferred_element_type=jnp.float32) * scale
        total = total + lax.optimization_barrier(term.astype(jnp.bfloat16)).astype(jnp.float32)
    return total

def reference(tokens, first_gain, value_weight, gate_weight, value_scale, gate_scale, conv_taps, chan_gain, mixout_weight, mixout_scale, second_gain, up_weight, up_scale, down_weight, down_scale):
    normed = rms_rows(tokens, first_gain)
    value_sum = jnp.dot(normed, value_weight.astype(jnp.bfloat16), preferred_element_type=jnp.float32)
    gate_sum = jnp.dot(normed, gate_weight.astype(jnp.bfloat16), preferred_element_type=jnp.float32)
    glu = value_sum * rounded(value_scale) * jax.nn.sigmoid(gate_sum * rounded(gate_scale))
    conv = causal_conv(glu, conv_taps)
    mean = lax.optimization_barrier(jnp.mean(conv, axis=1, keepdims=True))
    centred = conv - mean
    var = lax.optimization_barrier(jnp.mean(centred * centred, axis=1, keepdims=True))
    mixed_in = jax.nn.silu(centred * lax.rsqrt(var + 1e-05) * chan_gain).astype(jnp.bfloat16)
    mix_sum = block_sum(mixed_in, mixout_weight.astype(jnp.bfloat16), rounded(mixout_scale))
    middle = (tokens.astype(jnp.float32) + mix_sum).astype(jnp.bfloat16)
    normed2 = rms_rows(middle, second_gain)
    up_sum = jnp.dot(normed2, up_weight.astype(jnp.bfloat16), preferred_element_type=jnp.float32)
    hidden = jnp.square(jax.nn.relu(up_sum * rounded(up_scale))).astype(jnp.bfloat16)
    down_sum = block_sum(hidden, down_weight.astype(jnp.bfloat16), rounded(down_scale))
    return (middle.astype(jnp.float32) + down_sum).astype(jnp.bfloat16)
```

```python
import jax
import jax.numpy as jnp
from jax import lax
from jax.sharding import Mesh
from jax.sharding import PartitionSpec as P

SEQ_LEN = 128
FS = ("z", "y")
REP_FS = ("rep", "z", "y")
TP = ("x", "core")
RING = ("rep", "z")
F32 = jnp.float32
BF16 = jnp.bfloat16


def rounded(scale):
    return scale.astype(BF16).astype(F32)


def exchange(x, axis):
    return lax.all_to_all(x, axis, split_axis=0, concat_axis=0, tiled=True)


def copies_from(x, axis):
    return exchange(jnp.broadcast_to(x, (lax.axis_size(axis), *x.shape)), axis)


def shifted(x, distance):
    n = lax.axis_size(RING)
    return lax.ppermute(x, RING, [((i + distance) % n, i) for i in range(n)])


def ring_window(block):
    n = lax.axis_size("z")
    at = lax.axis_index("z")
    whole = jnp.zeros((n, *block.shape), block.dtype)
    whole = lax.dynamic_update_index_in_dim(whole, block, at, 0)
    for d in (4, -3, 3, -2, 2, -1, 1):
        whole = lax.dynamic_update_index_in_dim(whole, shifted(block, d), (at + d) % n, 0)
    return whole


def summed(x, axis):
    n = lax.axis_size(axis)
    blocks = exchange(x.reshape(n, x.shape[0] // n, x.shape[1]), axis)
    return blocks.astype(F32).sum(axis=0)


def tp_scattered(x):
    part = summed(x.astype(BF16), "core").astype(BF16)
    return summed(part, "x")


def tp_gathered(rows):
    part = copies_from(rows, "x")
    part = part.reshape(-1, rows.shape[1])
    return copies_from(part, "core").reshape(-1, rows.shape[1])


def own_rows(x):
    n = x.shape[0] // lax.axis_size(TP)
    block = lax.axis_index("core") * lax.axis_size("x") + lax.axis_index("x")
    return lax.dynamic_slice_in_dim(x, block * n, n, 0)


def rms_rows(rows, gain):
    values = rows.astype(F32)
    scaled = values * lax.rsqrt(jnp.mean(values * values, axis=-1, keepdims=True) + 1e-05)
    return (scaled * gain).astype(BF16)


def causal_conv(signal, taps):
    width = signal.shape[1]
    seqs = signal.reshape(-1, SEQ_LEN, width)
    result = lax.conv_general_dilated(
        seqs,
        taps[:, None, :],
        (1,),
        [(taps.shape[0] - 1, 0)],
        dimension_numbers=("NWC", "WIO", "NWC"),
        feature_group_count=width,
        precision=lax.Precision.HIGHEST,
    )
    return result.reshape(signal.shape)


def channel_stats(conv):
    width = conv.shape[1]
    total = jnp.sum(conv, axis=1)
    centred = conv - (total / width)[:, None]
    spread = jnp.sum(centred * centred, axis=1)
    both = lax.all_gather(jnp.stack([total, spread]), TP)
    n = both.shape[0]
    mean = both[:, 0].sum(axis=0) / (n * width)
    off = both[:, 0] / width - mean
    var = (both[:, 1].sum(axis=0) + width * (off * off).sum(axis=0)) / (n * width)
    return mean, var


def dot_t(a, b):
    return lax.dot_general(a, b, (((1,), (1,)), ((), ())), preferred_element_type=F32)


def on_device(
    tokens,
    first_gain,
    value_weight,
    gate_weight,
    value_scale,
    gate_scale,
    conv_taps,
    chan_gain,
    mixout_weight,
    mixout_scale,
    second_gain,
    up_weight,
    up_scale,
    down_weight,
    down_scale,
):
    rep = lax.axis_index("rep")
    reps = lax.axis_size("rep")
    width = value_weight.shape[1]
    mix_t = (mixout_weight.astype(BF16).astype(F32) * rounded(mixout_scale)).astype(BF16).T
    down_t = (down_weight.astype(BF16).astype(F32) * rounded(down_scale)).astype(BF16).T
    half = up_weight.shape[1] // reps
    up_half = lax.dynamic_slice_in_dim(up_weight, rep * half, half, 1).astype(BF16)
    down_half = lax.dynamic_slice_in_dim(down_t, rep * half, half, 1)
    ffn = lax.all_gather(jnp.concatenate([up_half, down_half], axis=1), REP_FS, axis=0, tiled=True)

    glu_local = jnp.concatenate([value_weight.astype(BF16), gate_weight.astype(BF16)], axis=1)
    glu_whole = ring_window(copies_from(glu_local, "y")).reshape(-1, 2 * width)
    mix_whole = ring_window(copies_from(mix_t, "y")).reshape(-1, width)

    normed = rms_rows(tokens, first_gain)
    sums = jnp.dot(normed, glu_whole, preferred_element_type=F32)
    glu = sums[:, :width] * rounded(value_scale) * jax.nn.sigmoid(sums[:, width:] * rounded(gate_scale))
    conv = causal_conv(glu, conv_taps)
    mean, var = channel_stats(conv)
    mixed_in = jax.nn.silu((conv - mean[:, None]) * lax.rsqrt(var[:, None] + 1e-05) * chan_gain).astype(BF16)
    mix_sum = tp_scattered(dot_t(mixed_in, mix_whole))
    middle = (own_rows(tokens).astype(F32) + mix_sum).astype(BF16)
    normed2 = tp_gathered(rms_rows(middle, second_gain))

    rows = ffn.shape[0] // reps
    up_mult = rounded(up_scale)
    down_sum = 0.0
    for r in range(reps):
        part = ffn[r * rows : (r + 1) * rows]
        up_sum = jnp.dot(normed2, part[:, :half], preferred_element_type=F32)
        hidden = jnp.square(jax.nn.relu(up_sum * up_mult[r * half : (r + 1) * half])).astype(BF16)
        down_sum = down_sum + dot_t(hidden, part[:, half:])
    layer_out = (middle.astype(F32) + tp_scattered(down_sum)).astype(BF16)
    return tp_gathered(layer_out)


def solution(mesh):
    torus = Mesh(
        mesh.devices.reshape(mesh.shape["rep"], 8, 4, 4, 2),
        ("rep", "z", "y", "x", "core"),
    )
    placed = (
        P(REP_FS, None),
        P(),
        P(FS, TP),
        P(FS, TP),
        P(TP),
        P(TP),
        P(None, TP),
        P(TP),
        P(TP, FS),
        P(FS),
        P(),
        P(FS, TP),
        P(TP),
        P(TP, FS),
        P(FS),
    )
    return jax.shard_map(
        on_device, mesh=torus, in_specs=placed, out_specs=P(REP_FS, None), check_vma=False
    )
```

```python
import jax
import jax.numpy as jnp
from jax import lax
from jax.sharding import Mesh
from jax.sharding import PartitionSpec as P


SEQ_LEN = 128
FS = ("z", "y")
REP_FS = ("rep", "z", "y")
TP = ("x", "core")
RING = ("rep", "z")
F32 = jnp.float32
BF16 = jnp.bfloat16


def rounded(scale):
    return scale.astype(BF16).astype(F32)


def exchange(x, axis):
    return lax.all_to_all(x, axis, split_axis=0, concat_axis=0, tiled=True)


def copies_from(x, axis):
    return exchange(jnp.broadcast_to(x, (lax.axis_size(axis), *x.shape)), axis)


def shifted(x, distance):
    n = lax.axis_size(RING)
    return lax.ppermute(x, RING, [((i + distance) % n, i) for i in range(n)])


def y_ring(block):
    n = lax.axis_size("y")
    at = lax.axis_index("y")
    whole = jnp.zeros((n, *block.shape), block.dtype)
    whole = lax.dynamic_update_index_in_dim(whole, block, at, 0)
    for d in (2, 1, 3):
        other = lax.ppermute(block, "y", [((i + d) % n, i) for i in range(n)])
        whole = lax.dynamic_update_index_in_dim(whole, other, (at + d) % n, 0)
    return whole


def ring_window(block):
    n = lax.axis_size("z")
    at = lax.axis_index("z")
    cut = block.shape[0] // 2
    whole = jnp.zeros((n, *block.shape), block.dtype)
    whole = lax.dynamic_update_index_in_dim(whole, block, at, 0)
    ahead = behind = block
    for d in range(1, n // 2):
        ahead = shifted(ahead, 1)
        behind = shifted(behind, -1)
        whole = lax.dynamic_update_index_in_dim(whole, ahead, (at + d) % n, 0)
        whole = lax.dynamic_update_index_in_dim(whole, behind, (at - d) % n, 0)
    ahead = shifted(ahead[:cut], 1)
    behind = shifted(behind[cut:], -1)
    last = jnp.concatenate([ahead, behind])
    return lax.dynamic_update_index_in_dim(whole, last, (at + n // 2) % n, 0)


def fs_copies(x):
    by_z = copies_from(x, "z")
    by_y = copies_from(by_z, "y")
    return by_y.swapaxes(0, 1).reshape(-1, x.shape[1])


def summed(x, axis):
    n = lax.axis_size(axis)
    blocks = exchange(x.reshape(n, x.shape[0] // n, x.shape[1]), axis)
    return blocks.astype(F32).sum(axis=0)


def tp_scattered(x):
    part = summed(x.astype(BF16), "core").astype(BF16)
    return summed(part, "x")


def tp_gathered(rows):
    part = copies_from(rows, "x").reshape(-1, rows.shape[1])
    return copies_from(part, "core").reshape(-1, rows.shape[1])


def own_rows(x):
    n = x.shape[0] // lax.axis_size(TP)
    block = lax.axis_index("core") * lax.axis_size("x") + lax.axis_index("x")
    return lax.dynamic_slice_in_dim(x, block * n, n, 0)


def rms_rows(rows, gain):
    values = rows.astype(F32)
    scaled = values * lax.rsqrt(jnp.mean(values * values, axis=-1, keepdims=True) + 1e-05)
    return (scaled * gain).astype(BF16)


def causal_conv(signal, taps):
    width = signal.shape[1]
    seqs = signal.reshape(-1, SEQ_LEN, width)
    result = lax.conv_general_dilated(
        seqs,
        taps[:, None, :],
        (1,),
        [(taps.shape[0] - 1, 0)],
        dimension_numbers=("NWC", "WIO", "NWC"),
        feature_group_count=width,
        precision=lax.Precision.HIGHEST,
    )
    return result.reshape(signal.shape)


def channel_stats(conv):
    width = conv.shape[1]
    total = jnp.sum(conv, axis=1)
    centred = conv - (total / width)[:, None]
    spread = jnp.sum(centred * centred, axis=1)
    both = lax.all_gather(jnp.stack([total, spread]), TP)
    n = both.shape[0]
    mean = both[:, 0].sum(axis=0) / (n * width)
    off = both[:, 0] / width - mean
    var = (both[:, 1].sum(axis=0) + width * (off * off).sum(axis=0)) / (n * width)
    return mean, var


def dot_t(a, b):
    return lax.dot_general(a, b, (((1,), (1,)), ((), ())), preferred_element_type=F32)


def on_device(
    tokens,
    first_gain,
    value_weight,
    gate_weight,
    value_scale,
    gate_scale,
    conv_taps,
    chan_gain,
    mixout_weight,
    mixout_scale,
    second_gain,
    up_weight,
    up_scale,
    down_weight,
    down_scale,
):
    rep = lax.axis_index("rep")
    reps = lax.axis_size("rep")
    width = value_weight.shape[1]
    mix_t = (mixout_weight.astype(BF16).astype(F32) * rounded(mixout_scale)).astype(BF16).T
    down_t = (down_weight.astype(BF16).astype(F32) * rounded(down_scale)).astype(BF16).T
    glu_local = jnp.concatenate([value_weight.astype(BF16), gate_weight.astype(BF16)], axis=1)
    glu_whole = fs_copies(glu_local)
    mix_whole = fs_copies(mix_t)

    hid = up_weight.shape[1]
    early = hid // 2
    half = (hid - early) // reps
    late = lax.dynamic_slice_in_dim(down_t, early + rep * half, half, 1)
    late = lax.all_gather(jnp.pad(late, ((0, 0), (0, (-half) % 512))), RING, axis=0)[:, :, :half]
    late = lax.all_gather(late, "y")
    near = jnp.concatenate([up_weight.astype(BF16), down_t[:, :early]], axis=1)
    near = ring_window(y_ring(near)).reshape(-1, hid + early)
    zs = lax.axis_size("z")
    late = [late[:, r * zs : (r + 1) * zs].swapaxes(0, 1).reshape(-1, half) for r in range(reps)]

    normed = rms_rows(tokens, first_gain)
    sums = jnp.dot(normed, glu_whole, preferred_element_type=F32)
    glu = sums[:, :width] * rounded(value_scale) * jax.nn.sigmoid(sums[:, width:] * rounded(gate_scale))
    conv = causal_conv(glu, conv_taps)
    mean, var = channel_stats(conv)
    mixed_in = jax.nn.silu((conv - mean[:, None]) * lax.rsqrt(var[:, None] + 1e-05) * chan_gain).astype(BF16)
    mix_sum = tp_scattered(dot_t(mixed_in, mix_whole))
    middle = (own_rows(tokens).astype(F32) + mix_sum).astype(BF16)
    normed2 = tp_gathered(rms_rows(middle, second_gain))

    up_sum = jnp.dot(normed2, near[:, :hid], preferred_element_type=F32)
    hidden = jnp.square(jax.nn.relu(up_sum * rounded(up_scale))).astype(BF16)
    down_sum = dot_t(hidden[:, :early], near[:, hid:])
    for r in range(reps):
        at = early + r * half
        down_sum = down_sum + dot_t(hidden[:, at : at + half], late[r])
    layer_out = (middle.astype(F32) + tp_scattered(down_sum)).astype(BF16)
    return tp_gathered(layer_out)


def solution(mesh):
    torus = Mesh(
        mesh.devices.reshape(mesh.shape["rep"], 8, 4, 4, 2),
        ("rep", "z", "y", "x", "core"),
    )
    placed = (
        P(REP_FS, None),
        P(),
        P(FS, TP),
        P(FS, TP),
        P(TP),
        P(TP),
        P(None, TP),
        P(TP),
        P(TP, FS),
        P(FS),
        P(),
        P(FS, TP),
        P(TP),
        P(TP, FS),
        P(FS),
    )

    return jax.shard_map(
        on_device, mesh=torus, in_specs=placed, out_specs=P(REP_FS, None), check_vma=False
    )
```

```python
import jax
import jax.numpy as jnp
from jax import lax
from jax.sharding import Mesh
from jax.sharding import PartitionSpec as P


SEQ_LEN = 128
FS = ("z", "y")
REP_FS = ("rep", "z", "y")
TP = ("x", "core")
RING = ("rep", "z")
F32 = jnp.float32
BF16 = jnp.bfloat16


def rounded(scale):
    return scale.astype(BF16).astype(F32)


def exchange(x, axis):
    return lax.all_to_all(x, axis, split_axis=0, concat_axis=0, tiled=True)


def copies_from(x, axis):
    return exchange(jnp.broadcast_to(x, (lax.axis_size(axis), *x.shape)), axis)


def shifted(x, distance):
    n = lax.axis_size(RING)
    return lax.ppermute(x, RING, [((i + distance) % n, i) for i in range(n)])


def y_ring(block):
    n = lax.axis_size("y")
    others = {}
    for d in (2, 1, 3):
        others[d] = lax.ppermute(block, "y", [((i + d) % n, i) for i in range(n)])
    return jnp.stack([block, others[1], others[2], others[3]])


def ring_window(block):
    n = lax.axis_size("z")
    cut = block.shape[0] // 2
    pieces = {0: block}
    ahead = behind = block
    for d in range(1, n // 2):
        ahead = shifted(ahead, 1)
        behind = shifted(behind, -1)
        pieces[d], pieces[n - d] = ahead, behind
    ahead = shifted(ahead[:cut], 1)
    behind = shifted(behind[cut:], -1)
    pieces[n // 2] = jnp.concatenate([ahead, behind])
    return [pieces[d] for d in range(n)]


def rolled(x, shift, axis):
    return lax.dynamic_slice_in_dim(jnp.concatenate([x, x], axis=axis), shift, x.shape[axis], axis)


def to_relative(x):
    zs, ys = lax.axis_size("z"), lax.axis_size("y")
    x = rolled(x, lax.axis_index("z") * (x.shape[1] // zs), 1).reshape(x.shape[0], zs, -1)
    return rolled(x, lax.axis_index("y") * (x.shape[2] // ys), 2).reshape(x.shape[0], -1)


def from_relative(x):
    zs, ys = lax.axis_size("z"), lax.axis_size("y")
    x = x.reshape(x.shape[0], zs, -1)
    x = rolled(x, (ys - lax.axis_index("y")) % ys * (x.shape[2] // ys), 2).reshape(x.shape[0], -1)
    return rolled(x, (zs - lax.axis_index("z")) % zs * (x.shape[1] // zs), 1)


def fs_copies(x):
    by_z = copies_from(x, "z")
    by_y = copies_from(by_z, "y")
    return by_y.swapaxes(0, 1).reshape(-1, x.shape[1])


def summed(x, axis):
    n = lax.axis_size(axis)
    blocks = exchange(x.reshape(n, x.shape[0] // n, x.shape[1]), axis)
    return blocks.astype(F32).sum(axis=0)


def tp_scattered(x):
    part = summed(x.astype(BF16), "core").astype(BF16)
    return summed(part, "x")


def tp_gathered(rows):
    part = copies_from(rows, "x").reshape(-1, rows.shape[1])
    return copies_from(part, "core").reshape(-1, rows.shape[1])


def own_rows(x):
    n = x.shape[0] // lax.axis_size(TP)
    block = lax.axis_index("core") * lax.axis_size("x") + lax.axis_index("x")
    return lax.dynamic_slice_in_dim(x, block * n, n, 0)


def rms_rows(rows, gain):
    values = rows.astype(F32)
    scaled = values * lax.rsqrt(jnp.mean(values * values, axis=-1, keepdims=True) + 1e-05)
    return (scaled * gain).astype(BF16)


def causal_conv(signal, taps):
    width = signal.shape[1]
    seqs = signal.reshape(-1, SEQ_LEN, width)
    result = lax.conv_general_dilated(
        seqs,
        taps[:, None, :],
        (1,),
        [(taps.shape[0] - 1, 0)],
        dimension_numbers=("NWC", "WIO", "NWC"),
        feature_group_count=width,
        precision=lax.Precision.HIGHEST,
    )
    return result.reshape(signal.shape)


def channel_stats(conv):
    width = conv.shape[1]
    total = jnp.sum(conv, axis=1)
    centred = conv - (total / width)[:, None]
    spread = jnp.sum(centred * centred, axis=1)
    both = lax.all_gather(jnp.stack([total, spread]), TP)
    n = both.shape[0]
    mean = both[:, 0].sum(axis=0) / (n * width)
    off = both[:, 0] / width - mean
    var = (both[:, 1].sum(axis=0) + width * (off * off).sum(axis=0)) / (n * width)
    return mean, var


def dot_t(a, b):
    return lax.dot_general(a, b, (((1,), (1,)), ((), ())), preferred_element_type=F32)


def on_device(
    tokens,
    first_gain,
    value_weight,
    gate_weight,
    value_scale,
    gate_scale,
    conv_taps,
    chan_gain,
    mixout_weight,
    mixout_scale,
    second_gain,
    up_weight,
    up_scale,
    down_weight,
    down_scale,
):
    width = value_weight.shape[1]
    hid = up_weight.shape[1]
    mix_t = (mixout_weight.astype(BF16).astype(F32) * rounded(mixout_scale)).astype(BF16).T
    down_t = (down_weight.astype(BF16).astype(F32) * rounded(down_scale)).astype(BF16).T
    conv_local = jnp.concatenate([value_weight.astype(BF16), gate_weight.astype(BF16), mix_t], axis=1)
    conv_whole = fs_copies(conv_local)
    pieces = ring_window(y_ring(jnp.concatenate([up_weight.astype(BF16), down_t], axis=1)))
    pieces = [p.reshape(-1, 2 * hid) for p in pieces]

    normed = rms_rows(tokens, first_gain)
    sums = jnp.dot(normed, conv_whole[:, : 2 * width], preferred_element_type=F32)
    glu = sums[:, :width] * rounded(value_scale) * jax.nn.sigmoid(sums[:, width:] * rounded(gate_scale))
    conv = causal_conv(glu, conv_taps)
    mean, var = channel_stats(conv)
    mixed_in = jax.nn.silu((conv - mean[:, None]) * lax.rsqrt(var[:, None] + 1e-05) * chan_gain).astype(BF16)
    mix_sum = tp_scattered(dot_t(mixed_in, conv_whole[:, 2 * width :]))
    middle = (own_rows(tokens).astype(F32) + mix_sum).astype(BF16)
    normed2 = tp_gathered(to_relative(rms_rows(middle, second_gain)))

    rows = pieces[0].shape[0]
    up_sum = 0.0
    for d in (0, 1, 7, 2, 6, 3, 5, 4):
        part = normed2[:, d * rows : (d + 1) * rows]
        up_sum = up_sum + jnp.dot(part, pieces[d][:, :hid], preferred_element_type=F32)
    hidden = jnp.square(jax.nn.relu(up_sum * rounded(up_scale))).astype(BF16)
    down_sum = jnp.concatenate([dot_t(hidden, p[:, hid:]).astype(BF16) for p in pieces], axis=1)
    layer_out = (middle.astype(F32) + from_relative(tp_scattered(down_sum))).astype(BF16)
    return tp_gathered(layer_out)


def solution(mesh):
    torus = Mesh(
        mesh.devices.reshape(mesh.shape["rep"], 8, 4, 4, 2),
        ("rep", "z", "y", "x", "core"),
    )
    placed = (
        P(REP_FS, None),
        P(),
        P(FS, TP),
        P(FS, TP),
        P(TP),
        P(TP),
        P(None, TP),
        P(TP),
        P(TP, FS),
        P(FS),
        P(),
        P(FS, TP),
        P(TP),
        P(TP, FS),
        P(FS),
    )

    return jax.shard_map(
        on_device, mesh=torus, in_specs=placed, out_specs=P(REP_FS, None), check_vma=False
    )
```

```python
import jax
import jax.numpy as jnp
from jax import lax
from jax.experimental import pallas as pl
from jax.experimental.pallas import tpu as pltpu
from jax.sharding import Mesh
from jax.sharding import PartitionSpec as P


SEQ_LEN = 128
FS = ("z", "y")
REP_FS = ("rep", "z", "y")
TP = ("x", "core")
RING = ("rep", "z")
F32 = jnp.float32
BF16 = jnp.bfloat16


def rounded(scale):
    return scale.astype(BF16).astype(F32)


def exchange(x, axis):
    return lax.all_to_all(x, axis, split_axis=0, concat_axis=0, tiled=True)


def copies_from(x, axis):
    return exchange(jnp.broadcast_to(x, (lax.axis_size(axis), *x.shape)), axis)


def shifted(x, distance):
    n = lax.axis_size(RING)
    return lax.ppermute(x, RING, [((i + distance) % n, i) for i in range(n)])


def y_ring(block):
    n = lax.axis_size("y")
    others = {}
    for d in (2, 1, 3):
        others[d] = lax.ppermute(block, "y", [((i + d) % n, i) for i in range(n)])
    return [block, others[1], others[2], others[3]]


def ring_window(chunks):
    n = lax.axis_size("z")
    ahead, behind, pieces = {}, {}, {}
    for name, block in chunks.items():
        ahead[name] = behind[name] = block
        pieces[name] = {0: block}
    for d in range(1, n // 2):
        for name in chunks:
            ahead[name] = pieces[name][d] = shifted(ahead[name], 1)
            behind[name] = pieces[name][n - d] = shifted(behind[name], -1)
    lists = []
    for name, block in chunks.items():
        cut = block.shape[0] // 2
        first = shifted(ahead[name][:cut], 1)
        second = shifted(behind[name][cut:], -1)
        got = pieces[name]
        ordered = [got[d] for d in range(n // 2)] + [first, second] + [got[d] for d in range(n // 2 + 1, n)]
        lists.append([p.reshape(-1, p.shape[-1]) for p in ordered])
    return lists


def rolled(x, shift, axis):
    return lax.dynamic_slice_in_dim(jnp.concatenate([x, x], axis=axis), shift, x.shape[axis], axis)


def to_relative(x):
    zs, ys = lax.axis_size("z"), lax.axis_size("y")
    x = rolled(x, lax.axis_index("z") * (x.shape[1] // zs), 1).reshape(x.shape[0], zs, -1)
    return rolled(x, lax.axis_index("y") * (x.shape[2] // ys), 2).reshape(x.shape[0], -1)


def from_relative(x):
    zs, ys = lax.axis_size("z"), lax.axis_size("y")
    x = x.reshape(x.shape[0], zs, -1)
    x = rolled(x, (ys - lax.axis_index("y")) % ys * (x.shape[2] // ys), 2).reshape(x.shape[0], -1)
    return rolled(x, (zs - lax.axis_index("z")) % zs * (x.shape[1] // zs), 1)


def fs_copies(x):
    by_z = copies_from(x, "z")
    by_y = copies_from(by_z, "y")
    return by_y.swapaxes(0, 1).reshape(-1, x.shape[1])


def swapped(x):
    return lax.ppermute(x, "core", [(0, 1), (1, 0)])


def x_scattered(mine, theirs):
    half = (mine + theirs.astype(F32)).astype(BF16)
    n = lax.axis_size("x")
    blocks = exchange(half.reshape(n, half.shape[0] // n, half.shape[1]), "x")
    return blocks.astype(F32).sum(axis=0)


def x_gathered(rows):
    return copies_from(rows, "x").reshape(-1, rows.shape[1])


def own_rows(x):
    n = x.shape[0] // lax.axis_size(TP)
    block = lax.axis_index("core") * lax.axis_size("x") + lax.axis_index("x")
    return lax.dynamic_slice_in_dim(x, block * n, n, 0)


def rms_rows(rows, gain):
    values = rows.astype(F32)
    scaled = values * lax.rsqrt(jnp.mean(values * values, axis=-1, keepdims=True) + 1e-05)
    return (scaled * gain).astype(BF16)


def causal_conv(signal, taps):
    width = signal.shape[1]
    seqs = signal.reshape(-1, SEQ_LEN, width)
    result = lax.conv_general_dilated(
        seqs,
        taps[:, None, :],
        (1,),
        [(taps.shape[0] - 1, 0)],
        dimension_numbers=("NWC", "WIO", "NWC"),
        feature_group_count=width,
        precision=lax.Precision.HIGHEST,
    )
    return result.reshape(signal.shape)


def channel_stats(conv):
    width = conv.shape[1]
    total = jnp.sum(conv, axis=1)
    centred = conv - (total / width)[:, None]
    spread = jnp.sum(centred * centred, axis=1)
    both = copies_from(jnp.stack([total, spread]), TP)
    n = both.shape[0]
    mean = both[:, 0].sum(axis=0) / (n * width)
    off = both[:, 0] / width - mean
    var = (both[:, 1].sum(axis=0) + width * (off * off).sum(axis=0)) / (n * width)
    return mean, var


def dot_t(a, b):
    return lax.dot_general(a, b, (((1,), (1,)), ((), ())), preferred_element_type=F32)


def ffn_body(count, *refs):
    mine, theirs, scale = refs[:3]
    ups, downs = refs[3 : 3 + count], refs[3 + count : 3 + 2 * count]
    out_mine, out_theirs, x, up, down, x_sems, up_sems, down_sems = refs[3 + 2 * count :]
    half = mine.shape[0]

    def fetch(pieces, whole, sems):
        at, copies = 0, []
        for i, piece in enumerate(pieces):
            n = piece.shape[0]
            copies.append((at, n, pltpu.make_async_copy(piece, whole.at[pl.ds(at, n)], sems.at[i])))
            at += n
        for _, _, copy in copies:
            copy.start()
        return copies

    x_copies = fetch((mine, theirs), x, x_sems)
    up_copies = fetch(ups, up, up_sems)
    down_copies = fetch(downs, down, down_sems)
    for _, _, copy in x_copies:
        copy.wait()
    total = None
    k = 0
    for i, (at, n, copy) in enumerate(up_copies):
        copy.wait()
        if i in (3, count - 1):
            part = jnp.dot(x[:, k : at + n], up[k : at + n, :], preferred_element_type=F32)
            total = part if total is None else total + part
            k = at + n
    hidden = jnp.square(jnp.maximum(total * scale[...], 0.0)).astype(BF16)
    k = 0
    for i, (at, n, copy) in enumerate(down_copies):
        copy.wait()
        if i in (1, 3, 6, count - 1):
            part = dot_t(hidden, down[k : at + n, :])
            out_mine[:, k : at + n] = part[:half]
            out_theirs[:, k : at + n] = part[half:].astype(BF16)
            k = at + n


def ffn(mine, theirs, scale, ups, downs):
    half, model = mine.shape
    hid = scale.shape[0]
    count = len(ups)
    anywhere = pl.BlockSpec(memory_space=pl.ANY)
    inside = pl.BlockSpec(memory_space=pltpu.VMEM)
    return pl.pallas_call(
        lambda *refs: ffn_body(count, *refs),
        in_specs=[anywhere, anywhere, inside] + [anywhere] * (2 * count),
        out_specs=[inside, inside],
        out_shape=[jax.ShapeDtypeStruct((half, model), F32), jax.ShapeDtypeStruct((half, model), BF16)],
        scratch_shapes=[
            pltpu.VMEM((2 * half, model), BF16),
            pltpu.VMEM((model, hid), BF16),
            pltpu.VMEM((model, hid), BF16),
            pltpu.SemaphoreType.DMA((2,)),
            pltpu.SemaphoreType.DMA((count,)),
            pltpu.SemaphoreType.DMA((count,)),
        ],
        cost_estimate=pl.CostEstimate(flops=8 * half * model * hid, bytes_accessed=4 * model * hid, transcendentals=0),
        name="ffn",
    )(mine, theirs, scale.reshape(1, hid), *ups, *downs)


def on_device(
    tokens,
    first_gain,
    value_weight,
    gate_weight,
    value_scale,
    gate_scale,
    conv_taps,
    chan_gain,
    mixout_weight,
    mixout_scale,
    second_gain,
    up_weight,
    up_scale,
    down_weight,
    down_scale,
):
    width = value_weight.shape[1]
    hid = up_weight.shape[1]
    mix_t = (mixout_weight.astype(BF16).astype(F32) * rounded(mixout_scale)).astype(BF16).T
    down_t = (down_weight.astype(BF16).astype(F32) * rounded(down_scale)).astype(BF16).T
    conv_local = jnp.concatenate([value_weight.astype(BF16), gate_weight.astype(BF16), mix_t], axis=1)
    conv_whole = fs_copies(conv_local)
    near = y_ring(jnp.concatenate([up_weight.astype(BF16), down_t], axis=1))
    chunks = {"up": jnp.stack([b[:, :hid] for b in near]), "down": jnp.stack([b[:, hid:] for b in near])}
    ups, downs = ring_window(chunks)

    normed = rms_rows(tokens, first_gain)
    sums = jnp.dot(normed, conv_whole[:, : 2 * width], preferred_element_type=F32)
    glu = sums[:, :width] * rounded(value_scale) * jax.nn.sigmoid(sums[:, width:] * rounded(gate_scale))
    conv = causal_conv(glu, conv_taps)
    mean, var = channel_stats(conv)
    mixed_in = jax.nn.silu((conv - mean[:, None]) * lax.rsqrt(var[:, None] + 1e-05) * chan_gain).astype(BF16)
    core = lax.axis_index("core")
    half = mixed_in.shape[0] // 2
    mix_whole = conv_whole[:, 2 * width :]
    sent = dot_t(lax.dynamic_slice_in_dim(mixed_in, (1 - core) * half, half, 0), mix_whole).astype(BF16)
    kept = dot_t(lax.dynamic_slice_in_dim(mixed_in, core * half, half, 0), mix_whole)
    mix_sum = x_scattered(kept, swapped(sent))
    middle = (own_rows(tokens).astype(F32) + mix_sum).astype(BF16)
    mine = x_gathered(to_relative(rms_rows(middle, second_gain)))
    kept, sent = ffn(mine, swapped(mine), rounded(up_scale), ups, downs)
    down_sum = from_relative(x_scattered(kept, swapped(sent)))
    mine = x_gathered((middle.astype(F32) + down_sum).astype(BF16))
    theirs = swapped(mine)
    first = core == 0
    return jnp.concatenate([jnp.where(first, mine, theirs), jnp.where(first, theirs, mine)])


def solution(mesh):
    torus = Mesh(
        mesh.devices.reshape(mesh.shape["rep"], 8, 4, 4, 2),
        ("rep", "z", "y", "x", "core"),
    )
    placed = (
        P(REP_FS, None),
        P(),
        P(FS, TP),
        P(FS, TP),
        P(TP),
        P(TP),
        P(None, TP),
        P(TP),
        P(TP, FS),
        P(FS),
        P(),
        P(FS, TP),
        P(TP),
        P(TP, FS),
        P(FS),
    )

    return jax.shard_map(on_device, mesh=torus, in_specs=placed, out_specs=P(REP_FS, None), check_vma=False)
```

```python
import jax
import jax.numpy as jnp
from jax import lax
from jax.experimental import pallas as pl
from jax.experimental.pallas import tpu as pltpu
from jax.sharding import Mesh
from jax.sharding import PartitionSpec as P


SEQ_LEN = 128
FS = ("z", "y")
REP_FS = ("rep", "z", "y")
TP = ("x", "core")
RING = ("rep", "z")
F32 = jnp.float32
BF16 = jnp.bfloat16


def rounded(scale):
    return scale.astype(BF16).astype(F32)


def exchange(x, axis):
    return lax.all_to_all(x, axis, split_axis=0, concat_axis=0, tiled=True)


def copies_from(x, axis):
    return exchange(jnp.broadcast_to(x, (lax.axis_size(axis), *x.shape)), axis)


def y_ring(block):
    n = lax.axis_size("y")
    others = {}
    for d in (2, 1, 3):
        others[d] = lax.ppermute(block, "y", [((i + d) % n, i) for i in range(n)])
    return [block, others[1], others[2], others[3]]


def hop(x):
    n = lax.axis_size(RING)
    pairs = [((2 * ((i + 1) % n)), 2 * i) for i in range(n)] + [(2 * ((i - 1) % n) + 1, 2 * i + 1) for i in range(n)]
    return lax.ppermute(x, (*RING, "core"), pairs)


def side_ring(chunks):
    core = lax.axis_index("core")
    pieces = {}
    for name, block in chunks.items():
        pieces[name] = [jnp.stack([block, swapped(block)])]
    for d in range(1, 5):
        for got in pieces.values():
            last = got[-1]
            if d == 4:
                last = lax.dynamic_slice_in_dim(last, core * (last.shape[1] // 2), last.shape[1] // 2, 1)
            got.append(hop(last))
    return [[p.reshape(2, -1, p.shape[-1]) for p in got] for got in pieces.values()]


def to_sides(x):
    w = x.shape[1] // 16
    at = lambda a, b: x[:, a * w : b * w]
    ahead = jnp.concatenate([at(0, 1), at(2, 9)], axis=1)
    behind = jnp.concatenate([at(1, 2), at(14, 16), at(12, 14), at(10, 12), at(9, 10)], axis=1)
    return ahead, behind


def from_sides(ahead, behind):
    w = ahead.shape[1] // 8
    at = lambda a, b: behind[:, a * w : b * w]
    return jnp.concatenate(
        [ahead[:, :w], at(0, 1), ahead[:, w:], at(7, 8), at(5, 7), at(3, 5), at(1, 3)], axis=1
    )


def rolled(x, shift, axis):
    return lax.dynamic_slice_in_dim(jnp.concatenate([x, x], axis=axis), shift, x.shape[axis], axis)


def to_relative(x):
    zs, ys = lax.axis_size("z"), lax.axis_size("y")
    x = rolled(x, lax.axis_index("z") * (x.shape[1] // zs), 1).reshape(x.shape[0], zs, -1)
    return rolled(x, lax.axis_index("y") * (x.shape[2] // ys), 2).reshape(x.shape[0], -1)


def from_relative(x):
    zs, ys = lax.axis_size("z"), lax.axis_size("y")
    x = x.reshape(x.shape[0], zs, -1)
    x = rolled(x, (ys - lax.axis_index("y")) % ys * (x.shape[2] // ys), 2).reshape(x.shape[0], -1)
    return rolled(x, (zs - lax.axis_index("z")) % zs * (x.shape[1] // zs), 1)


def fs_copies(x):
    by_z = copies_from(x, "z")
    by_y = copies_from(by_z, "y")
    return by_y.swapaxes(0, 1).reshape(-1, x.shape[1])


def swapped(x):
    return lax.ppermute(x, "core", [(0, 1), (1, 0)])


def x_scattered(mine, theirs):
    half = (mine + theirs.astype(F32)).astype(BF16)
    n = lax.axis_size("x")
    blocks = exchange(half.reshape(n, half.shape[0] // n, half.shape[1]), "x")
    return blocks.astype(F32).sum(axis=0)


def x_gathered(rows):
    return copies_from(rows, "x").reshape(-1, rows.shape[1])


def own_rows(x):
    n = x.shape[0] // lax.axis_size(TP)
    block = lax.axis_index("core") * lax.axis_size("x") + lax.axis_index("x")
    return lax.dynamic_slice_in_dim(x, block * n, n, 0)


def rms_rows(rows, gain):
    values = rows.astype(F32)
    scaled = values * lax.rsqrt(jnp.mean(values * values, axis=-1, keepdims=True) + 1e-05)
    return (scaled * gain).astype(BF16)


def causal_conv(signal, taps):
    width = signal.shape[1]
    seqs = signal.reshape(-1, SEQ_LEN, width)
    result = lax.conv_general_dilated(
        seqs,
        taps[:, None, :],
        (1,),
        [(taps.shape[0] - 1, 0)],
        dimension_numbers=("NWC", "WIO", "NWC"),
        feature_group_count=width,
        precision=lax.Precision.HIGHEST,
    )
    return result.reshape(signal.shape)


def channel_stats(conv):
    width = conv.shape[1]
    total = jnp.sum(conv, axis=1)
    centred = conv - (total / width)[:, None]
    spread = jnp.sum(centred * centred, axis=1)
    both = copies_from(jnp.stack([total, spread]), TP)
    n = both.shape[0]
    mean = both[:, 0].sum(axis=0) / (n * width)
    off = both[:, 0] / width - mean
    var = (both[:, 1].sum(axis=0) + width * (off * off).sum(axis=0)) / (n * width)
    return mean, var


def dot_t(a, b):
    return lax.dot_general(a, b, (((1,), (1,)), ((), ())), preferred_element_type=F32)


def fetch_side(slot, core, pieces, whole, sems):
    half = pieces[0].shape[1] // 2
    sources = [pieces[0].at[slot, pl.ds(core * half, half)]] + [p.at[slot] for p in pieces[1:]]
    at, copies = 0, []
    for i, source in enumerate(sources):
        n = source.shape[0]
        copies.append(pltpu.make_async_copy(source, whole.at[pl.ds(at, n)], sems.at[i]))
        copies[-1].start()
        at += n
    return copies


def up_body(slot, core_ref, own, theirs, *refs):
    pieces, (out, x, w, x_sems, w_sems) = refs[:-5], refs[-5:]
    core = core_ref[0]
    n = own.shape[0]
    copies = [
        pltpu.make_async_copy(own, x.at[pl.ds(core * n, n)], x_sems.at[0]),
        pltpu.make_async_copy(theirs, x.at[pl.ds((1 - core) * n, n)], x_sems.at[1]),
    ]
    for copy in copies:
        copy.start()
    for copy in copies + fetch_side(slot, core, pieces, w, w_sems):
        copy.wait()
    out[...] = jnp.dot(x[...], w[...], preferred_element_type=F32).astype(out.dtype)


def down_body(slot, core_ref, hidden, acc, *refs):
    pieces, (out, w, w_sems) = refs[:-3], refs[-3:]
    for copy in fetch_side(slot, core_ref[0], pieces, w, w_sems):
        copy.wait()
    part = dot_t(hidden[...], w[...])
    if slot == 0:
        out[...] = part
        return
    part = (part + acc[...]).astype(out.dtype)
    blocks, halves, n, _ = out.shape
    for i in range(blocks):
        for j in range(halves):
            at = (j * blocks + i) * n
            out[i, j] = part[at : at + n]


def side_call(body, name, slot, core, operands, pieces, out_shape, scratch):
    anywhere = pl.BlockSpec(memory_space=pl.ANY)
    inside = pl.BlockSpec(memory_space=pltpu.VMEM)
    here = anywhere if name == "up" else inside
    cols = pieces[0].shape[2]
    rows = 4 * pieces[0].shape[1]
    return pl.pallas_call(
        lambda *refs: body(slot, *refs),
        in_specs=[pl.BlockSpec(memory_space=pltpu.SMEM)] + [here] * len(operands) + [anywhere] * len(pieces),
        out_specs=inside,
        out_shape=out_shape,
        scratch_shapes=scratch + [pltpu.VMEM((rows, cols), BF16)]
        + ([pltpu.SemaphoreType.DMA((2,))] if name == "up" else [])
        + [pltpu.SemaphoreType.DMA((len(pieces),))],
        cost_estimate=pl.CostEstimate(flops=512 * rows * cols, bytes_accessed=2 * rows * cols, transcendentals=0),
    )(core.reshape(1), *operands, *pieces)


def ffn(own, theirs, core, scale, ups, downs):
    tokens, cols = 2 * own.shape[0], own.shape[1]
    hid = scale.shape[0]
    up = lambda slot, kind: side_call(
        up_body, "up", slot, core, (own, theirs), ups,
        jax.ShapeDtypeStruct((tokens, hid), kind), [pltpu.VMEM((tokens, cols), BF16)],
    )
    sent = swapped(up(1, BF16))
    up_sum = up(0, F32) + sent.astype(F32)
    hidden = jnp.square(jax.nn.relu(up_sum * scale)).astype(BF16)
    other = swapped(hidden)
    kept = side_call(
        down_body, "down", 0, core, (hidden, hidden), downs, jax.ShapeDtypeStruct((tokens, cols), F32), []
    )
    n = lax.axis_size("x")
    blocks = jax.ShapeDtypeStruct((n, 2, tokens // (2 * n), cols), BF16)
    return side_call(down_body, "down", 1, core, (other, kept), downs, blocks, [])


def on_device(
    tokens,
    first_gain,
    value_weight,
    gate_weight,
    value_scale,
    gate_scale,
    conv_taps,
    chan_gain,
    mixout_weight,
    mixout_scale,
    second_gain,
    up_weight,
    up_scale,
    down_weight,
    down_scale,
):
    width = value_weight.shape[1]
    hid = up_weight.shape[1]
    mix_t = (mixout_weight.astype(BF16).astype(F32) * rounded(mixout_scale)).astype(BF16).T
    down_t = (down_weight.astype(BF16).astype(F32) * rounded(down_scale)).astype(BF16).T
    conv_local = jnp.concatenate([value_weight.astype(BF16), gate_weight.astype(BF16), mix_t], axis=1)
    conv_whole = fs_copies(conv_local)
    near = y_ring(jnp.concatenate([up_weight.astype(BF16), down_t], axis=1))
    chunks = {"up": jnp.stack([b[:, :hid] for b in near]), "down": jnp.stack([b[:, hid:] for b in near])}
    ups, downs = side_ring(chunks)

    normed = rms_rows(tokens, first_gain)
    sums = jnp.dot(normed, conv_whole[:, : 2 * width], preferred_element_type=F32)
    glu = sums[:, :width] * rounded(value_scale) * jax.nn.sigmoid(sums[:, width:] * rounded(gate_scale))
    conv = causal_conv(glu, conv_taps)
    mean, var = channel_stats(conv)
    mixed_in = jax.nn.silu((conv - mean[:, None]) * lax.rsqrt(var[:, None] + 1e-05) * chan_gain).astype(BF16)
    core = lax.axis_index("core")
    half = mixed_in.shape[0] // 2
    mix_whole = conv_whole[:, 2 * width :]
    sent = dot_t(lax.dynamic_slice_in_dim(mixed_in, (1 - core) * half, half, 0), mix_whole).astype(BF16)
    kept = dot_t(lax.dynamic_slice_in_dim(mixed_in, core * half, half, 0), mix_whole)
    mix_sum = x_scattered(kept, swapped(sent))
    middle = (own_rows(tokens).astype(F32) + mix_sum).astype(BF16)
    sides = jnp.stack(to_sides(to_relative(rms_rows(middle, second_gain))))
    sides = copies_from(sides, "x")
    cols = sides.shape[-1]
    side_of = lambda c: lax.dynamic_index_in_dim(sides, c, 1, keepdims=False).reshape(-1, cols)
    theirs = swapped(side_of(1 - core))
    blocks = ffn(side_of(core), theirs, core, rounded(up_scale), ups, downs)
    blocks = exchange(blocks, "x").astype(F32).sum(axis=0)
    kept = lax.dynamic_index_in_dim(blocks, core, 0, keepdims=False)
    sent = lax.dynamic_index_in_dim(blocks, 1 - core, 0, keepdims=False).astype(BF16)
    got = swapped(sent).astype(F32)
    first = core == 0
    down_sum = from_relative(from_sides(jnp.where(first, kept, got), jnp.where(first, got, kept)))
    mine = x_gathered((middle.astype(F32) + down_sum).astype(BF16))
    theirs = swapped(mine)
    return jnp.concatenate([jnp.where(first, mine, theirs), jnp.where(first, theirs, mine)])


def solution(mesh):
    torus = Mesh(
        mesh.devices.reshape(mesh.shape["rep"], 8, 4, 4, 2),
        ("rep", "z", "y", "x", "core"),
    )
    placed = (
        P(REP_FS, None),
        P(),
        P(FS, TP),
        P(FS, TP),
        P(TP),
        P(TP),
        P(None, TP),
        P(TP),
        P(TP, FS),
        P(FS),
        P(),
        P(FS, TP),
        P(TP),
        P(TP, FS),
        P(FS),
    )

    return jax.shard_map(on_device, mesh=torus, in_specs=placed, out_specs=P(REP_FS, None), check_vma=False)
```

```python
import jax
import jax.numpy as jnp
from jax import lax
from jax.experimental import pallas as pl
from jax.experimental.pallas import tpu as pltpu
from jax.sharding import Mesh
from jax.sharding import PartitionSpec as P


SEQ_LEN = 128
FS = ("z", "y")
REP_FS = ("rep", "z", "y")
TP = ("x", "core")
RING = ("rep", "z")
F32 = jnp.float32
BF16 = jnp.bfloat16


def rounded(scale):
    return scale.astype(BF16).astype(F32)


def exchange(x, axis):
    return lax.all_to_all(x, axis, split_axis=0, concat_axis=0, tiled=True)


def copies_from(x, axis):
    return exchange(jnp.broadcast_to(x, (lax.axis_size(axis), *x.shape)), axis)


def y_ring(block):
    n = lax.axis_size("y")
    others = {}
    for d in (2, 1, 3):
        others[d] = lax.ppermute(block, "y", [((i + d) % n, i) for i in range(n)])
    return [block, others[1], others[2], others[3]]


def hop(x):
    n = lax.axis_size(RING)
    pairs = [((2 * ((i + 1) % n)), 2 * i) for i in range(n)] + [(2 * ((i - 1) % n) + 1, 2 * i + 1) for i in range(n)]
    return lax.ppermute(x, (*RING, "core"), pairs)


def side_ring(chunks):
    core = lax.axis_index("core")
    pieces = {}
    for name, block in chunks.items():
        pieces[name] = [block, swapped(block)]
    for d in range(1, 5):
        for got in pieces.values():
            last = jnp.stack(got) if d == 1 else got[-1]
            if d == 4:
                last = lax.dynamic_slice_in_dim(last, core * (last.shape[1] // 2), last.shape[1] // 2, 1)
            got.append(hop(last))
    return [
        [p.reshape(-1, p.shape[-1]) for p in got[:2]] + [p.reshape(2, -1, p.shape[-1]) for p in got[2:]]
        for got in pieces.values()
    ]


def to_sides(x):
    w = x.shape[1] // 16
    at = lambda a, b: x[:, a * w : b * w]
    ahead = jnp.concatenate([at(0, 1), at(2, 9)], axis=1)
    behind = jnp.concatenate([at(1, 2), at(14, 16), at(12, 14), at(10, 12), at(9, 10)], axis=1)
    return ahead, behind


def from_sides(ahead, behind):
    w = ahead.shape[1] // 8
    at = lambda a, b: behind[:, a * w : b * w]
    return jnp.concatenate(
        [ahead[:, :w], at(0, 1), ahead[:, w:], at(7, 8), at(5, 7), at(3, 5), at(1, 3)], axis=1
    )


def rolled(x, shift, axis):
    return lax.dynamic_slice_in_dim(jnp.concatenate([x, x], axis=axis), shift, x.shape[axis], axis)


def to_relative(x):
    zs, ys = lax.axis_size("z"), lax.axis_size("y")
    x = rolled(x, lax.axis_index("z") * (x.shape[1] // zs), 1).reshape(x.shape[0], zs, -1)
    return rolled(x, lax.axis_index("y") * (x.shape[2] // ys), 2).reshape(x.shape[0], -1)


def from_relative(x):
    zs, ys = lax.axis_size("z"), lax.axis_size("y")
    x = x.reshape(x.shape[0], zs, -1)
    x = rolled(x, (ys - lax.axis_index("y")) % ys * (x.shape[2] // ys), 2).reshape(x.shape[0], -1)
    return rolled(x, (zs - lax.axis_index("z")) % zs * (x.shape[1] // zs), 1)


def fs_copies(x):
    by_z = copies_from(x, "z")
    by_y = copies_from(by_z, "y")
    return by_y.swapaxes(0, 1).reshape(-1, x.shape[1])


def swapped(x):
    return lax.ppermute(x, "core", [(0, 1), (1, 0)])


def x_scattered(mine, theirs):
    half = (mine + theirs.astype(F32)).astype(BF16)
    n = lax.axis_size("x")
    blocks = exchange(half.reshape(n, half.shape[0] // n, half.shape[1]), "x")
    return blocks.astype(F32).sum(axis=0)


def x_gathered(rows):
    return copies_from(rows, "x").reshape(-1, rows.shape[1])


def own_rows(x):
    n = x.shape[0] // lax.axis_size(TP)
    block = lax.axis_index("core") * lax.axis_size("x") + lax.axis_index("x")
    return lax.dynamic_slice_in_dim(x, block * n, n, 0)


def rms_rows(rows, gain):
    values = rows.astype(F32)
    scaled = values * lax.rsqrt(jnp.mean(values * values, axis=-1, keepdims=True) + 1e-05)
    return (scaled * gain).astype(BF16)


def causal_conv(signal, taps):
    width = signal.shape[1]
    seqs = signal.reshape(-1, SEQ_LEN, width)
    result = lax.conv_general_dilated(
        seqs,
        taps[:, None, :],
        (1,),
        [(taps.shape[0] - 1, 0)],
        dimension_numbers=("NWC", "WIO", "NWC"),
        feature_group_count=width,
        precision=lax.Precision.HIGHEST,
    )
    return result.reshape(signal.shape)


def channel_stats(conv):
    width = conv.shape[1]
    total = jnp.sum(conv, axis=1)
    centred = conv - (total / width)[:, None]
    spread = jnp.sum(centred * centred, axis=1)
    both = copies_from(jnp.stack([total, spread]), TP)
    n = both.shape[0]
    mean = both[:, 0].sum(axis=0) / (n * width)
    off = both[:, 0] / width - mean
    var = (both[:, 1].sum(axis=0) + width * (off * off).sum(axis=0)) / (n * width)
    return mean, var


def dot_t(a, b):
    return lax.dot_general(a, b, (((1,), (1,)), ((), ())), preferred_element_type=F32)


def fetch_side(slot, core, pieces, whole, sems):
    half = pieces[0].shape[0] // 2
    sources = [pieces[0].at[pl.ds(core * half, half)]] + [p.at[slot] for p in pieces[1:]]
    at, copies = 0, []
    for i, source in enumerate(sources):
        n = source.shape[0]
        copies.append(pltpu.make_async_copy(source, whole.at[pl.ds(at, n)], sems.at[i]))
        copies[-1].start()
        at += n
    return copies


def up_body(slot, core_ref, own, theirs, *refs):
    pieces, (out, x, w, x_sems, w_sems) = refs[:-5], refs[-5:]
    core = core_ref[0]
    n = own.shape[0]
    copies = [
        pltpu.make_async_copy(own, x.at[pl.ds(core * n, n)], x_sems.at[0]),
        pltpu.make_async_copy(theirs, x.at[pl.ds((1 - core) * n, n)], x_sems.at[1]),
    ]
    for copy in copies:
        copy.start()
    for copy in copies + fetch_side(slot, core, pieces, w, w_sems):
        copy.wait()
    out[...] = jnp.dot(x[...], w[...], preferred_element_type=F32).astype(out.dtype)


def down_body(slot, core_ref, hidden, acc, *refs):
    pieces, (out, w, w_sems) = refs[:-3], refs[-3:]
    for copy in fetch_side(slot, core_ref[0], pieces, w, w_sems):
        copy.wait()
    part = dot_t(hidden[...], w[...])
    if slot == 0:
        out[...] = part
        return
    part = (part + acc[...]).astype(out.dtype)
    blocks, halves, n, _ = out.shape
    for i in range(blocks):
        for j in range(halves):
            at = (j * blocks + i) * n
            out[i, j] = part[at : at + n]


def side_call(body, name, slot, core, operands, pieces, out_shape, scratch):
    anywhere = pl.BlockSpec(memory_space=pl.ANY)
    inside = pl.BlockSpec(memory_space=pltpu.VMEM)
    pieces = [pieces[slot]] + pieces[2:]
    here = anywhere if name == "up" else inside
    cols = pieces[0].shape[1]
    rows = 4 * pieces[0].shape[0]
    return pl.pallas_call(
        lambda *refs: body(slot, *refs),
        in_specs=[pl.BlockSpec(memory_space=pltpu.SMEM)] + [here] * len(operands) + [anywhere] * len(pieces),
        out_specs=inside,
        out_shape=out_shape,
        scratch_shapes=scratch + [pltpu.VMEM((rows, cols), BF16)]
        + ([pltpu.SemaphoreType.DMA((2,))] if name == "up" else [])
        + [pltpu.SemaphoreType.DMA((len(pieces),))],
        cost_estimate=pl.CostEstimate(flops=512 * rows * cols, bytes_accessed=2 * rows * cols, transcendentals=0),
    )(core.reshape(1), *operands, *pieces)


def ffn(own, theirs, core, scale, ups, downs):
    tokens, cols = 2 * own.shape[0], own.shape[1]
    hid = scale.shape[0]
    up = lambda slot, kind: side_call(
        up_body, "up", slot, core, (own, theirs), ups,
        jax.ShapeDtypeStruct((tokens, hid), kind), [pltpu.VMEM((tokens, cols), BF16)],
    )
    sent = swapped(up(1, BF16))
    up_sum = up(0, F32) + sent.astype(F32)
    hidden = jnp.square(jax.nn.relu(up_sum * scale)).astype(BF16)
    other = swapped(hidden)
    kept = side_call(
        down_body, "down", 0, core, (hidden, hidden), downs, jax.ShapeDtypeStruct((tokens, cols), F32), []
    )
    n = lax.axis_size("x")
    blocks = jax.ShapeDtypeStruct((n, 2, tokens // (2 * n), cols), BF16)
    return side_call(down_body, "down", 1, core, (other, kept), downs, blocks, [])


def on_device(
    tokens,
    first_gain,
    value_weight,
    gate_weight,
    value_scale,
    gate_scale,
    conv_taps,
    chan_gain,
    mixout_weight,
    mixout_scale,
    second_gain,
    up_weight,
    up_scale,
    down_weight,
    down_scale,
):
    width = value_weight.shape[1]
    hid = up_weight.shape[1]
    mix_t = (mixout_weight.astype(BF16).astype(F32) * rounded(mixout_scale)).astype(BF16).T
    down_t = (down_weight.astype(BF16).astype(F32) * rounded(down_scale)).astype(BF16).T
    conv_local = jnp.concatenate([value_weight.astype(BF16), gate_weight.astype(BF16), mix_t], axis=1)
    conv_whole = fs_copies(conv_local)
    near = y_ring(jnp.concatenate([up_weight.astype(BF16), down_t], axis=1))
    chunks = {"up": jnp.stack([b[:, :hid] for b in near]), "down": jnp.stack([b[:, hid:] for b in near])}
    ups, downs = side_ring(chunks)

    normed = rms_rows(tokens, first_gain)
    sums = jnp.dot(normed, conv_whole[:, : 2 * width], preferred_element_type=F32)
    glu = sums[:, :width] * rounded(value_scale) * jax.nn.sigmoid(sums[:, width:] * rounded(gate_scale))
    conv = causal_conv(glu, conv_taps)
    mean, var = channel_stats(conv)
    mixed_in = jax.nn.silu((conv - mean[:, None]) * lax.rsqrt(var[:, None] + 1e-05) * chan_gain).astype(BF16)
    core = lax.axis_index("core")
    half = mixed_in.shape[0] // 2
    mix_whole = conv_whole[:, 2 * width :]
    sent = dot_t(lax.dynamic_slice_in_dim(mixed_in, (1 - core) * half, half, 0), mix_whole).astype(BF16)
    kept = dot_t(lax.dynamic_slice_in_dim(mixed_in, core * half, half, 0), mix_whole)
    mix_sum = x_scattered(kept, swapped(sent))
    middle = (own_rows(tokens).astype(F32) + mix_sum).astype(BF16)
    sides = jnp.stack(to_sides(to_relative(rms_rows(middle, second_gain))))
    sides = copies_from(sides, "x")
    cols = sides.shape[-1]
    side_of = lambda c: lax.dynamic_index_in_dim(sides, c, 1, keepdims=False).reshape(-1, cols)
    theirs = swapped(side_of(1 - core))
    blocks = ffn(side_of(core), theirs, core, rounded(up_scale), ups, downs)
    blocks = exchange(blocks, "x").astype(F32).sum(axis=0)
    kept = lax.dynamic_index_in_dim(blocks, core, 0, keepdims=False)
    sent = lax.dynamic_index_in_dim(blocks, 1 - core, 0, keepdims=False).astype(BF16)
    got = swapped(sent).astype(F32)
    first = core == 0
    down_sum = from_relative(from_sides(jnp.where(first, kept, got), jnp.where(first, got, kept)))
    mine = x_gathered((middle.astype(F32) + down_sum).astype(BF16))
    theirs = swapped(mine)
    return jnp.concatenate([jnp.where(first, mine, theirs), jnp.where(first, theirs, mine)])


def solution(mesh):
    torus = Mesh(
        mesh.devices.reshape(mesh.shape["rep"], 8, 4, 4, 2),
        ("rep", "z", "y", "x", "core"),
    )
    placed = (
        P(REP_FS, None),
        P(),
        P(FS, TP),
        P(FS, TP),
        P(TP),
        P(TP),
        P(None, TP),
        P(TP),
        P(TP, FS),
        P(FS),
        P(),
        P(FS, TP),
        P(TP),
        P(TP, FS),
        P(FS),
    )

    return jax.shard_map(on_device, mesh=torus, in_specs=placed, out_specs=P(REP_FS, None), check_vma=False)
```

```python
import jax
import jax.numpy as jnp
from jax import lax
from jax.experimental import pallas as pl
from jax.experimental.pallas import tpu as pltpu
from jax.sharding import Mesh
from jax.sharding import PartitionSpec as P


SEQ_LEN = 128
FS = ("z", "y")
REP_FS = ("rep", "z", "y")
TP = ("x", "core")
RING = ("rep", "z")
F32 = jnp.float32
BF16 = jnp.bfloat16


def rounded(scale):
    return scale.astype(BF16).astype(F32)


def exchange(x, axis):
    return lax.all_to_all(x, axis, split_axis=0, concat_axis=0, tiled=True)


def copies_from(x, axis):
    return exchange(jnp.broadcast_to(x, (lax.axis_size(axis), *x.shape)), axis)


def y_ring(block):
    n = lax.axis_size("y")
    others = {}
    for d in (2, 1, 3):
        others[d] = lax.ppermute(block, "y", [((i + d) % n, i) for i in range(n)])
    return [block, others[1], others[2], others[3]]


def hop(x):
    n = lax.axis_size(RING)
    pairs = [((2 * ((i + 1) % n)), 2 * i) for i in range(n)] + [(2 * ((i - 1) % n) + 1, 2 * i + 1) for i in range(n)]
    return lax.ppermute(x, (*RING, "core"), pairs)


def side_ring(chunks):
    core = lax.axis_index("core")
    pieces = {}
    for name, block in chunks.items():
        pieces[name] = [block, swapped(block)]
    for d in range(1, 5):
        for got in pieces.values():
            last = jnp.stack(got) if d == 1 else got[-1]
            if d == 4:
                last = lax.dynamic_slice_in_dim(last, core * (last.shape[1] // 2), last.shape[1] // 2, 1)
            got.append(hop(last))
    return [
        [p.reshape(-1, p.shape[-1]) for p in got[:2]] + [p.reshape(2, -1, p.shape[-1]) for p in got[2:]]
        for got in pieces.values()
    ]


def to_sides(x):
    w = x.shape[1] // 16
    at = lambda a, b: x[:, a * w : b * w]
    ahead = jnp.concatenate([at(0, 1), at(2, 9)], axis=1)
    behind = jnp.concatenate([at(1, 2), at(14, 16), at(12, 14), at(10, 12), at(9, 10)], axis=1)
    return ahead, behind


def from_sides(ahead, behind):
    w = ahead.shape[1] // 8
    at = lambda a, b: behind[:, a * w : b * w]
    return jnp.concatenate(
        [ahead[:, :w], at(0, 1), ahead[:, w:], at(7, 8), at(5, 7), at(3, 5), at(1, 3)], axis=1
    )


def rolled(x, shift, axis):
    return lax.dynamic_slice_in_dim(jnp.concatenate([x, x], axis=axis), shift, x.shape[axis], axis)


def to_relative(x):
    zs, ys = lax.axis_size("z"), lax.axis_size("y")
    x = rolled(x, lax.axis_index("z") * (x.shape[1] // zs), 1).reshape(x.shape[0], zs, -1)
    return rolled(x, lax.axis_index("y") * (x.shape[2] // ys), 2).reshape(x.shape[0], -1)


def from_relative(x):
    zs, ys = lax.axis_size("z"), lax.axis_size("y")
    x = x.reshape(x.shape[0], zs, -1)
    x = rolled(x, (ys - lax.axis_index("y")) % ys * (x.shape[2] // ys), 2).reshape(x.shape[0], -1)
    return rolled(x, (zs - lax.axis_index("z")) % zs * (x.shape[1] // zs), 1)


def fs_copies(x):
    by_z = copies_from(x, "z")
    by_y = copies_from(by_z, "y")
    return by_y.swapaxes(0, 1).reshape(-1, x.shape[1])


def swapped(x):
    return lax.ppermute(x, "core", [(0, 1), (1, 0)])


def x_scattered(mine, theirs):
    half = (mine + theirs.astype(F32)).astype(BF16)
    n = lax.axis_size("x")
    blocks = exchange(half.reshape(n, half.shape[0] // n, half.shape[1]), "x")
    return blocks.astype(F32).sum(axis=0)


def x_gathered(rows):
    return copies_from(rows, "x").reshape(-1, rows.shape[1])


def own_rows(x):
    n = x.shape[0] // lax.axis_size(TP)
    block = lax.axis_index("core") * lax.axis_size("x") + lax.axis_index("x")
    return lax.dynamic_slice_in_dim(x, block * n, n, 0)


def rms_rows(rows, gain):
    values = rows.astype(F32)
    scaled = values * lax.rsqrt(jnp.mean(values * values, axis=-1, keepdims=True) + 1e-05)
    return (scaled * gain).astype(BF16)


def causal_conv(signal, taps):
    width = signal.shape[1]
    seqs = signal.reshape(-1, SEQ_LEN, width)
    result = lax.conv_general_dilated(
        seqs,
        taps[:, None, :],
        (1,),
        [(taps.shape[0] - 1, 0)],
        dimension_numbers=("NWC", "WIO", "NWC"),
        feature_group_count=width,
        precision=lax.Precision.HIGHEST,
    )
    return result.reshape(signal.shape)


def channel_stats(conv):
    width = conv.shape[1]
    total = jnp.sum(conv, axis=1)
    centred = conv - (total / width)[:, None]
    spread = jnp.sum(centred * centred, axis=1)
    both = copies_from(jnp.stack([total, spread]), TP)
    n = both.shape[0]
    mean = both[:, 0].sum(axis=0) / (n * width)
    off = both[:, 0] / width - mean
    var = (both[:, 1].sum(axis=0) + width * (off * off).sum(axis=0)) / (n * width)
    return mean, var


def dot_t(a, b):
    return lax.dot_general(a, b, (((1,), (1,)), ((), ())), preferred_element_type=F32)


def fetch_side(slot, core, pieces, whole, sems):
    half = pieces[0].shape[0] // 2
    sources = [pieces[slot].at[pl.ds(core * half, half)]] + [p.at[slot] for p in pieces[2:]]
    at, copies = 0, []
    for i, source in enumerate(sources):
        n = source.shape[0]
        copies.append(pltpu.make_async_copy(source, whole.at[slot, pl.ds(at, n)], sems.at[slot, i]))
        copies[-1].start()
        at += n
    return copies


def up_body(core_ref, own, theirs, *refs):
    pieces, (kept, sent, x, w, x_sems, w_sems) = refs[:-6], refs[-6:]
    core = core_ref[0]
    n = own.shape[0]
    first = [
        pltpu.make_async_copy(own, x.at[pl.ds(core * n, n)], x_sems.at[0]),
        pltpu.make_async_copy(theirs, x.at[pl.ds((1 - core) * n, n)], x_sems.at[1]),
    ]
    for copy in first:
        copy.start()
    first += fetch_side(1, core, pieces, w, w_sems)
    second = fetch_side(0, core, pieces, w, w_sems)
    for copy in first:
        copy.wait()
    sent[...] = jnp.dot(x[...], w[1], preferred_element_type=F32).astype(sent.dtype)
    for copy in second:
        copy.wait()
    kept[...] = jnp.dot(x[...], w[0], preferred_element_type=F32)


def down_body(core_ref, hidden, other, *refs):
    pieces, (out, w, w_sems) = refs[:-3], refs[-3:]
    core = core_ref[0]
    first = fetch_side(0, core, pieces, w, w_sems)
    second = fetch_side(1, core, pieces, w, w_sems)
    for copy in first:
        copy.wait()
    part = dot_t(hidden[...], w[0])
    for copy in second:
        copy.wait()
    part = (part + dot_t(other[...], w[1])).astype(out.dtype)
    blocks, halves, n, _ = out.shape
    for i in range(blocks):
        for j in range(halves):
            at = (j * blocks + i) * n
            out[i, j] = part[at : at + n]


def side_call(body, core, operands, where, pieces, out_shape, scratch, more):
    anywhere = pl.BlockSpec(memory_space=pl.ANY)
    inside = pl.BlockSpec(memory_space=pltpu.VMEM)
    rows, cols = 4 * pieces[0].shape[0], pieces[0].shape[1]
    return pl.pallas_call(
        body,
        in_specs=[pl.BlockSpec(memory_space=pltpu.SMEM)] + [where] * len(operands) + [anywhere] * len(pieces),
        out_specs=jax.tree.map(lambda _: inside, out_shape),
        out_shape=out_shape,
        scratch_shapes=scratch
        + [pltpu.VMEM((2, rows, cols), BF16)]
        + more
        + [pltpu.SemaphoreType.DMA((2, len(pieces) - 1))],
        cost_estimate=pl.CostEstimate(flops=1024 * rows * cols, bytes_accessed=4 * rows * cols, transcendentals=0),
        compiler_params=pltpu.CompilerParams(vmem_limit_bytes=52 * 2**20),
    )(core.reshape(1), *operands, *pieces)


def ffn(own, theirs, core, scale, ups, downs):
    tokens, cols = 2 * own.shape[0], own.shape[1]
    hid = scale.shape[0]
    anywhere = pl.BlockSpec(memory_space=pl.ANY)
    inside = pl.BlockSpec(memory_space=pltpu.VMEM)
    shapes = [jax.ShapeDtypeStruct((tokens, hid), F32), jax.ShapeDtypeStruct((tokens, hid), BF16)]
    kept, sent = side_call(
        up_body, core, (own, theirs), anywhere, ups, shapes,
        [pltpu.VMEM((tokens, cols), BF16)], [pltpu.SemaphoreType.DMA((2,))],
    )
    up_sum = kept + swapped(sent).astype(F32)
    hidden = jnp.square(jax.nn.relu(up_sum * scale)).astype(BF16)
    n = lax.axis_size("x")
    blocks = jax.ShapeDtypeStruct((n, 2, tokens // (2 * n), cols), BF16)
    return side_call(down_body, core, (hidden, swapped(hidden)), inside, downs, blocks, [], [])


def on_device(
    tokens,
    first_gain,
    value_weight,
    gate_weight,
    value_scale,
    gate_scale,
    conv_taps,
    chan_gain,
    mixout_weight,
    mixout_scale,
    second_gain,
    up_weight,
    up_scale,
    down_weight,
    down_scale,
):
    width = value_weight.shape[1]
    hid = up_weight.shape[1]
    mix_t = (mixout_weight.astype(BF16).astype(F32) * rounded(mixout_scale)).astype(BF16).T
    down_t = (down_weight.astype(BF16).astype(F32) * rounded(down_scale)).astype(BF16).T
    conv_local = jnp.concatenate([value_weight.astype(BF16), gate_weight.astype(BF16), mix_t], axis=1)
    conv_whole = fs_copies(conv_local)
    near = y_ring(jnp.concatenate([up_weight.astype(BF16), down_t], axis=1))
    chunks = {"up": jnp.stack([b[:, :hid] for b in near]), "down": jnp.stack([b[:, hid:] for b in near])}
    ups, downs = side_ring(chunks)

    normed = rms_rows(tokens, first_gain)
    sums = jnp.dot(normed, conv_whole[:, : 2 * width], preferred_element_type=F32)
    glu = sums[:, :width] * rounded(value_scale) * jax.nn.sigmoid(sums[:, width:] * rounded(gate_scale))
    conv = causal_conv(glu, conv_taps)
    mean, var = channel_stats(conv)
    mixed_in = jax.nn.silu((conv - mean[:, None]) * lax.rsqrt(var[:, None] + 1e-05) * chan_gain).astype(BF16)
    core = lax.axis_index("core")
    half = mixed_in.shape[0] // 2
    mix_whole = conv_whole[:, 2 * width :]
    sent = dot_t(lax.dynamic_slice_in_dim(mixed_in, (1 - core) * half, half, 0), mix_whole).astype(BF16)
    kept = dot_t(lax.dynamic_slice_in_dim(mixed_in, core * half, half, 0), mix_whole)
    mix_sum = x_scattered(kept, swapped(sent))
    middle = (own_rows(tokens).astype(F32) + mix_sum).astype(BF16)
    sides = jnp.stack(to_sides(to_relative(rms_rows(middle, second_gain))))
    sides = copies_from(sides, "x")
    cols = sides.shape[-1]
    side_of = lambda c: lax.dynamic_index_in_dim(sides, c, 1, keepdims=False).reshape(-1, cols)
    theirs = swapped(side_of(1 - core))
    blocks = ffn(side_of(core), theirs, core, rounded(up_scale), ups, downs)
    blocks = exchange(blocks, "x").astype(F32).sum(axis=0)
    kept = lax.dynamic_index_in_dim(blocks, core, 0, keepdims=False)
    sent = lax.dynamic_index_in_dim(blocks, 1 - core, 0, keepdims=False).astype(BF16)
    got = swapped(sent).astype(F32)
    first = core == 0
    down_sum = from_relative(from_sides(jnp.where(first, kept, got), jnp.where(first, got, kept)))
    mine = x_gathered((middle.astype(F32) + down_sum).astype(BF16))
    theirs = swapped(mine)
    return jnp.concatenate([jnp.where(first, mine, theirs), jnp.where(first, theirs, mine)])


def solution(mesh):
    torus = Mesh(
        mesh.devices.reshape(mesh.shape["rep"], 8, 4, 4, 2),
        ("rep", "z", "y", "x", "core"),
    )
    placed = (
        P(REP_FS, None),
        P(),
        P(FS, TP),
        P(FS, TP),
        P(TP),
        P(TP),
        P(None, TP),
        P(TP),
        P(TP, FS),
        P(FS),
        P(),
        P(FS, TP),
        P(TP),
        P(TP, FS),
        P(FS),
    )

    return jax.shard_map(on_device, mesh=torus, in_specs=placed, out_specs=P(REP_FS, None), check_vma=False)
```
